512 devices in a mesh: sp: 64 (over z, y), tp: 8 (over x, core).
Axes of the slice: x: 4, y: 4, z: 16, core: 2. Of those that a mesh axis runs over, the one named last changes fastest.
Arguments:
- tokens: bfloat16 [6144, 4, 1024], P(('sp', 'tp')), may hold values from -6 to 6
- in_gain: float32 [1024], replicated, may hold values from 0.1 to 1.9
- w_query: bfloat16 [1024, 1024], P('sp', 'tp'), may hold values from -0.1875 to 0.1875
- w_key: bfloat16 [1024, 1024], P('sp', 'tp'), may hold values from -0.1875 to 0.1875
- w_value: bfloat16 [1024, 1024], P('sp', 'tp'), may hold values from -0.1875 to 0.1875
- w_gate: bfloat16 [1024, 1024], P('sp', 'tp'), may hold values from -0.1875 to 0.1875
- w_beta: bfloat16 [1024, 8], P('sp', 'tp'), may hold values from -0.1875 to 0.1875
- conv_query: bfloat16 [4, 1024], P(None, 'tp'), may hold values from -3 to 3
- conv_key: bfloat16 [4, 1024], P(None, 'tp'), may hold values from -3 to 3
- conv_value: bfloat16 [4, 1024], P(None, 'tp'), may hold values from -3 to 3
- decay_rate: float32 [8], P('tp'), may hold values from 0.1 to 3
- out_gain: float32 [128], replicated, may hold values from 0.1 to 1.9
- w_out: bfloat16 [1024, 1024], P('tp', 'sp'), may hold values from -0.1875 to 0.1875
Outputs:
- mixed: bfloat16 [6144, 4, 1024], P(('sp', 'tp'))
The draws below stay inside these ranges and needn't reach their ends.
All inputs are finite; a program needn't handle non-finite values.
Results may differ from the reference program's by a relative error of at most 0.02.
Values may be sent and summed in bfloat16 or wider, within the bound.
A program may use at most 64 MiB of HBM per device.

```python
import math
import jax
import jax.numpy as jnp
from jax import lax

D = 1024
HEADS = 8
DK = 128
CONV_K = 4
BLOCK = 32
SEQS = 4
TOKENS = 6144


def shard_levels(own_key, extent, shards, low, top_value):
    level, own = 1.0, jax.random.fold_in(own_key, 6)
    for dim, parts in shards:
        heights = jnp.exp(jax.random.uniform(jax.random.fold_in(own, dim), (parts,), jnp.float32, low / len(shards), top_value / len(shards)))
        level = level * jnp.repeat(heights, extent[dim] // parts).reshape([-1 if axis == dim else 1 for axis in range(len(extent))])
    return level


def normal_values(stream_key, shape, spread, limit, shards=(), held_as=jnp.bfloat16):
    values = spread * jax.random.normal(stream_key, shape, jnp.float32)
    if shards:
        values = values * shard_levels(stream_key, shape, shards, -0.22, 0.18)
    return jnp.clip(values, -limit, limit).astype(held_as)


def setup_inputs(seed: int = 0) -> dict:
    key_of = jax.random.split(jax.random.key(seed), 14)
    tokens = normal_values(key_of[0], (TOKENS, SEQS, D), 1.0, 6.0, ((0, 512),))
    in_gain = jnp.clip(1.0 + 0.18 * jax.random.normal(key_of[1], (D,), jnp.float32), 0.1, 1.9)
    w_query = normal_values(key_of[2], (D, HEADS * DK), D ** -0.5, 0.1875, ((0, 64), (1, 8)))
    w_key = normal_values(key_of[3], (D, HEADS * DK), D ** -0.5, 0.1875, ((0, 64), (1, 8)))
    w_value = normal_values(key_of[4], (D, HEADS * DK), D ** -0.5, 0.1875, ((0, 64), (1, 8)))
    w_gate = normal_values(key_of[5], (D, HEADS * DK), D ** -0.5, 0.1875, ((0, 64), (1, 8)))
    w_beta = normal_values(key_of[6], (D, HEADS), D ** -0.5, 0.1875, ((0, 64), (1, 8)))
    conv_query = normal_values(key_of[7], (CONV_K, HEADS * DK), CONV_K ** -0.5, 3.0, ((1, 8),))
    conv_key = normal_values(key_of[8], (CONV_K, HEADS * DK), CONV_K ** -0.5, 3.0, ((1, 8),))
    conv_value = normal_values(key_of[9], (CONV_K, HEADS * DK), CONV_K ** -0.5, 3.0, ((1, 8),))
    decay_rate = jnp.clip(jnp.exp(math.log(3.0) - 3.4011974 * jax.random.uniform(key_of[10], (HEADS,), jnp.float32) ** shard_levels(key_of[10], (HEADS,), ((0, 8),), -0.2, 0.2)), 0.1, 3.0)
    out_gain = jnp.clip(1.0 + 0.18 * jax.random.normal(key_of[11], (DK,), jnp.float32), 0.1, 1.9)
    w_out = normal_values(key_of[12], (HEADS * DK, D), (HEADS * DK) ** -0.5, 0.1875, ((0, 8), (1, 64)))
    return {"tokens": tokens, "in_gain": in_gain, "w_query": w_query, "w_key": w_key, "w_value": w_value, "w_gate": w_gate, "w_beta": w_beta, "conv_query": conv_query, "conv_key": conv_key, "conv_value": conv_value, "decay_rate": decay_rate, "out_gain": out_gain, "w_out": w_out}


epsilon = 1e-06
out_epsilon = 1e-10
highest = lax.Precision.HIGHEST

def unit_inverse(lower):
    size = lower.shape[-1]
    inverse = jnp.eye(size, dtype=jnp.float32) - lower
    power = jnp.matmul(lower, lower, precision=highest)
    span = 2
    while span < size:
        inverse = inverse + jnp.matmul(inverse, power, precision=highest)
        power = jnp.matmul(power, power, precision=highest)
        span = span * 2
    return inverse

def make_terms(query, keys, values, beta, rate_col):
    size = query.shape[-2]
    steps = jnp.arange(1, size + 1).astype(jnp.float32)
    cumulative = -rate_col * steps
    lower_mask = jnp.tril(jnp.ones((size, size), bool))
    strict_mask = jnp.tril(jnp.ones((size, size), bool), -1)
    decay = jnp.where(lower_mask, jnp.exp(cumulative[..., :, None] - cumulative[..., None, :]), 0.0)
    weighted = keys * beta[..., None]
    lower = jnp.where(strict_mask, jnp.einsum('...cd,...sd->...cs', weighted, keys, precision=highest) * decay, 0.0)
    inverse = unit_inverse(lower)
    update = jnp.einsum('...cs,...sv->...cv', inverse, values * beta[..., None], precision=highest)
    erase = jnp.einsum('...cs,...sd->...cd', inverse, weighted * jnp.exp(cumulative)[..., None], precision=highest)
    scores = jnp.einsum('...cd,...sd->...cs', query, keys, precision=highest) * decay
    query_decayed = query * jnp.exp(cumulative)[..., None]
    final = cumulative[..., -1:]
    keys_decayed = keys * jnp.exp(final - cumulative)[..., None]
    return (query_decayed, keys_decayed, update, erase, scores, jnp.exp(final))

def apply_block(state, terms):
    query_decayed, keys_decayed, update, erase, scores, kept = terms
    fresh = update - jnp.einsum('...cd,...dv->...cv', erase, state, precision=highest)
    output = jnp.einsum('...cd,...dv->...cv', query_decayed, state, precision=highest)
    output = output + jnp.einsum('...cs,...sv->...cv', scores, fresh, precision=highest)
    state = state * kept[..., None] + jnp.einsum('...cd,...cv->...dv', keys_decayed, fresh, precision=highest)
    return (state, output)

def causal_conv(pre, conv_taps, history):
    width = conv_taps.shape[0]
    extended = jnp.concatenate([history, pre], axis=0).astype(jnp.float32)
    length = pre.shape[0]
    total = jnp.zeros(pre.shape, jnp.float32)
    for tap in range(width):
        total = total + extended[tap:tap + length] * conv_taps[tap].astype(jnp.float32)
    return total

def rms_scale(values_in, gain):
    values = values_in.astype(jnp.float32)
    scaled = values * lax.rsqrt(lax.optimization_barrier(jnp.mean(values * values, axis=-1, keepdims=True)) + epsilon)
    return (scaled * gain).astype(jnp.bfloat16)

def l2_normalize(array):
    return array * lax.rsqrt(lax.optimization_barrier(jnp.sum(array * array, axis=-1, keepdims=True)) + epsilon)

def finish(outputs, out_gain, gate_pre):
    normed = outputs * lax.rsqrt(lax.optimization_barrier(jnp.mean(outputs * outputs, axis=-1, keepdims=True)) + out_epsilon) * out_gain
    gate = jax.nn.silu(gate_pre.astype(jnp.float32)).reshape(outputs.shape)
    return (normed * gate).astype(jnp.bfloat16).reshape(outputs.shape[0], outputs.shape[1], -1)

def reference(tokens, in_gain, w_query, w_key, w_value, w_gate, w_beta, conv_query, conv_key, conv_value, decay_rate, out_gain, w_out):
    width = tokens.shape[2]
    head_width = HEADS * DK
    normed = rms_scale(tokens, in_gain)
    flat = normed.reshape(-1, width)

    def project(weight):
        return jnp.dot(flat, weight, preferred_element_type=jnp.float32).astype(jnp.bfloat16).reshape(TOKENS, SEQS, -1)
    mixed_pre = jnp.concatenate([project(w_query), project(w_key), project(w_value)], axis=2)
    gate_pre = project(w_gate)
    beta_pre = project(w_beta)
    history = jnp.zeros((CONV_K - 1, SEQS, 3 * head_width), jnp.bfloat16)
    conv_taps = jnp.concatenate([conv_query, conv_key, conv_value], axis=1)
    convolved = jax.nn.silu(causal_conv(mixed_pre, conv_taps, history))

    def split_heads(array):
        return array.reshape(TOKENS, SEQS, HEADS, DK)
    query = l2_normalize(split_heads(convolved[:, :, :head_width])) * DK ** (-0.5)
    keys = l2_normalize(split_heads(convolved[:, :, head_width:2 * head_width]))
    values = split_heads(convolved[:, :, 2 * head_width:])
    beta = jax.nn.sigmoid(beta_pre.astype(jnp.float32) + math.log(DK / (4.0 * TOKENS)))
    rate_col = (decay_rate / TOKENS)[:, None]
    blocks = TOKENS // BLOCK

    def to_blocks(array):
        return jnp.moveaxis(array.reshape(blocks, BLOCK, SEQS, HEADS, DK), 1, 3)
    beta_blocks = jnp.moveaxis(beta.reshape(blocks, BLOCK, SEQS, HEADS), 1, 3)

    def advance(state, inputs):
        query_block, key_block, value_block, beta_block = inputs
        return apply_block(state, make_terms(query_block, key_block, value_block, beta_block, rate_col))
    initial = jnp.zeros((SEQS, HEADS, DK, DK), jnp.float32)
    _, outputs = lax.scan(advance, initial, (to_blocks(query), to_blocks(keys), to_blocks(values), beta_blocks))
    outputs = jnp.moveaxis(outputs, 3, 1).reshape(TOKENS, SEQS, HEADS, DK)
    gated = finish(outputs, out_gain, gate_pre)
    mixed = jnp.dot(gated.reshape(-1, head_width), w_out, preferred_element_type=jnp.float32).astype(jnp.bfloat16)
    return mixed.reshape(TOKENS, SEQS, width)
```

```python
import math

import jax
import jax.numpy as jnp
from jax import lax
from jax.experimental import pallas as pl
from jax.experimental.pallas import tpu as pltpu
from jax.sharding import PartitionSpec as P

MESH = pl.DeviceIdType.MESH
F32 = jnp.float32
BF16 = jnp.bfloat16

Z, Y, X, C = 16, 4, 4, 2
TP = X * C
ROWS = 16
PAD = 4
TOK = ROWS - PAD
PLANE = Y * TP
CHUNK = 128
CHUNKS = PLANE * ROWS // CHUNK
CHUNK_TOKENS = CHUNK // ROWS * TOK
TOKENS = 6144
D = 1024
DK = 128
WIDE = 5 * DK

epsilon = 1e-06
out_epsilon = 1e-10


def place():
    sp, tp = lax.axis_index("sp"), lax.axis_index("tp")
    return sp // Y, sp % Y, tp // C, tp % C


def at(z, y, x, c):
    return ((z + Z) % Z * Y + (y + Y) % Y, (x + X) % X * C + (c + C) % C)


def meet(peers):
    barrier = pltpu.get_barrier_semaphore()
    for peer in peers:
        pl.semaphore_signal(barrier, inc=1, device_id=peer, device_id_type=MESH)
    pl.semaphore_wait(barrier, len(peers))


def remote(src, dst, send, recv, peer):
    return pltpu.make_async_remote_copy(
        src_ref=src, dst_ref=dst, send_sem=send, recv_sem=recv, device_id=peer, device_id_type=MESH
    )


NEAR = (-1, 1, 2)


def gather_kernel(nrm, wblk, wob, xf, wf, wo, local, s_tok, r_tok, s_w, r_w, s_o, r_o):
    z, y, x, c = place()
    tp = x * C + c
    zh, zl = z // 4, z % 4
    meet(
        [at(z + k, y, x, c) for k in (-1, 1, -2, 2, 4, 8, 12)]
        + [at(z, y + k, x, c) for k in (1, 2, 3)]
        + [at(z, y, x + k, c) for k in (1, 2, 3)]
        + [at(z, y, x, c + 1)]
    )
    sent = []

    def go(copy):
        copy.start()
        sent.append(copy)
        return copy

    def block(ys, k):
        return xf.at[1 + (y + ys + Y) % Y * TP + (x + k + X) % X * C + c]

    own_x = xf.at[1 + y * TP + tp]
    w1 = [go(remote(wblk, wf.at[zh, zl, y], s_w.at[k], r_w.at[k], at(z + 4 * k + 4, y, x, c))) for k in range(3)]
    o1 = [go(remote(wob, wo.at[zh, zl, y], s_o.at[k], r_o.at[k], at(z + 4 * k + 4, y, x, c))) for k in range(3)]
    t1 = [
        go(remote(nrm.at[(y + k + 1) % Y], own_x, s_tok.at[k], r_tok.at[k], at(z, y + k + 1, x, c)))
        for k in range(3)
    ]
    t2, t3 = {}, {}

    def pass_x(ys, src):
        for k in range(3):
            i = 3 + ys * 3 + k
            t2[ys, k] = go(remote(src, block(-ys, 0), s_tok.at[i], r_tok.at[i], at(z, y, x + k + 1, c)))

    def pass_core(ys, k, src):
        i = 15 + ys * 4 + k
        t3[ys, k] = go(remote(src, block(-ys, -k), s_tok.at[i], r_tok.at[i], at(z, y, x, c + 1)))

    pass_x(0, nrm.at[y])
    pass_core(0, 0, nrm.at[y])
    mine = [
        pltpu.make_async_copy(wblk, wf.at[zh, zl, y], local.at[0]),
        pltpu.make_async_copy(wob, wo.at[zh, zl, y], local.at[1]),
        pltpu.make_async_copy(nrm.at[y], own_x, local.at[2]),
    ]
    for copy in mine:
        copy.start()
    for k in range(3):
        t1[k].wait_recv()
        pass_x(k + 1, block(-k - 1, 0))
        pass_core(k + 1, 0, block(-k - 1, 0))
    for ys in range(4):
        for k in range(3):
            t2[ys, k].wait_recv()
            pass_core(ys, k + 1, block(-ys, -k - 1))

    w3 = {}

    def pass_y(r, zr):
        for k in range(3):
            i = 6 + 3 * r + k
            part = wf.at[:, zr, y]
            w3[r, k] = go(remote(part, part, s_w.at[i], r_w.at[i], at(z, y + k + 1, x, c)))

    mine[0].wait()
    mine[1].wait()
    for copy in w1:
        copy.wait_recv()
    w2 = []
    for k, off in enumerate(NEAR):
        part = wf.at[:, zl, y]
        w2.append(go(remote(part, part, s_w.at[3 + k], r_w.at[3 + k], at(z + off, y, x, c))))
    pass_y(0, zl)
    for copy in o1:
        copy.wait_recv()
    o2 = []
    for k, off in enumerate(NEAR):
        part = wo.at[:, zl, y]
        o2.append(go(remote(part, part, s_o.at[3 + k], r_o.at[3 + k], at(z + off, y, x, c))))
    for k, off in enumerate(NEAR):
        w2[k].wait_recv()
        pass_y(k + 1, (z - off + Z) % 4)
    for copy in o2:
        copy.wait_recv()
    o3 = []
    for k in range(3):
        part = wo.at[:, :, y]
        o3.append(go(remote(part, part, s_o.at[6 + k], r_o.at[6 + k], at(z, y + k + 1, x, c))))

    mine[2].wait()
    for ys in range(4):
        for k in range(4):
            t3[ys, k].wait_recv()
    history = go(remote(xf.at[PLANE], xf.at[0], s_tok.at[31], r_tok.at[31], at(z + 1, y, x, c)))
    for copy in list(w3.values()) + o3 + [history]:
        copy.wait_recv()
    for copy in sent:
        copy.wait_send()


def gather(nrm, wblk, wob):
    vmem = pl.BlockSpec(memory_space=pltpu.VMEM)
    dma = pltpu.SemaphoreType.DMA
    return pl.pallas_call(
        gather_kernel,
        out_shape=(
            jax.ShapeDtypeStruct((PLANE + 1, ROWS, D), BF16),
            jax.ShapeDtypeStruct((4, 4, Y, 16, WIDE), BF16),
            jax.ShapeDtypeStruct((4, 4, Y, 16, DK), BF16),
        ),
        in_specs=[vmem] * 3,
        out_specs=(vmem,) * 3,
        scratch_shapes=[dma((3,)), dma((32,)), dma((32,)), dma((18,)), dma((18,)), dma((9,)), dma((9,))],
        compiler_params=pltpu.CompilerParams(collective_id=1, has_side_effects=True),
        name="gather",
    )(nrm, wblk, wob)


def mm(a, b, dims=((1,), (0,))):
    return lax.dot_general(a.astype(BF16), b.astype(BF16), (dims, ((), ())), preferred_element_type=F32)


def sigmoid(v):
    return 1.0 / (1.0 + jnp.exp(-v))


def local_kernel(rate, x, w, taps, maps, reach_out, local_out, gate_out, ext):
    pre = mm(x[...].reshape((PLANE + 1) * ROWS, D), w[...]).astype(BF16).astype(F32)
    total = PLANE * ROWS
    full = total + ROWS
    first = jnp.where(lax.axis_index("sp") // Y == 0, 0.0, 1.0).astype(F32)
    ext[...] = pre[:, : 3 * DK]
    ext[0:ROWS, :] = pre[:ROWS, : 3 * DK] * first
    gate_pre = pre[ROWS:, 3 * DK : 4 * DK]
    gate_out[...] = gate_pre * sigmoid(gate_pre)
    beta_pre = pre[ROWS:, 4 * DK : 4 * DK + 1]
    inner = lax.broadcasted_iota(jnp.int32, (total, 3 * DK), 0) % ROWS
    fixed = jnp.where(inner < PAD, ext[ROWS - PAD : full - PAD, :], ext[ROWS:full, :])
    ext[ROWS:full, :] = fixed
    conv = ext[ROWS:full, :] * taps[3:4, :]
    for k in range(1, 4):
        conv = conv + ext[ROWS - k : full - k, :] * taps[3 - k : 4 - k, :]
    conv = conv * sigmoid(conv)
    row = lax.broadcasted_iota(jnp.int32, (total, 1), 0)
    real = (row % ROWS >= PAD).astype(F32)
    q, k, v = conv[:, :DK], conv[:, DK : 2 * DK], conv[:, 2 * DK :]
    q = q * (lax.rsqrt(jnp.sum(q * q, axis=1, keepdims=True) + epsilon) * DK**-0.5)
    k = k * (lax.rsqrt(jnp.sum(k * k, axis=1, keepdims=True) + epsilon) * real)
    beta = sigmoid(beta_pre + math.log(DK / (4.0 * TOKENS))) * real

    lam = rate[0, 0] / TOKENS
    steps = lambda r: (r // ROWS * TOK + jnp.maximum(r % ROWS - (PAD - 1), 0)).astype(F32)
    ri = lax.broadcasted_iota(jnp.int32, (CHUNK, CHUNK), 0)
    ci = lax.broadcasted_iota(jnp.int32, (CHUNK, CHUNK), 1)
    decay = jnp.where(ri >= ci, jnp.exp(-lam * (steps(ri) - steps(ci))), 0.0)
    strict = jnp.where(ri > ci, decay, 0.0)
    in32 = ri // 32 == ci // 32
    in64 = ri // 64 == ci // 64
    eye = (ri == ci).astype(F32)
    here = steps(lax.broadcasted_iota(jnp.int32, (CHUNK, 1), 0))
    fall = jnp.exp(-lam * here)
    rest = jnp.exp(-lam * (CHUNK_TOKENS - here))
    kept = jnp.exp(jnp.full((1, 1), -1.0, F32) * lam * CHUNK_TOKENS)

    n = range(CHUNKS)
    cut = lambda a: [a[CHUNK * i : CHUNK * (i + 1)] for i in n]
    qs, ks, vs, bs = cut(q), cut(k), cut(v), cut(beta)
    ws = [ks[i] * bs[i] for i in n]
    both = [mm(jnp.concatenate([ws[i], qs[i]], axis=0), ks[i], ((1,), (1,))) for i in n]
    lower = [both[i][:CHUNK] * strict for i in n]
    scores = [both[i][CHUNK:] * decay for i in n]
    diag = [jnp.where(in32, lower[i], 0.0) for i in n]
    inverse = [eye - diag[i] for i in n]
    power = [mm(diag[i], diag[i]) for i in n]
    for step in range(4):
        inverse = [inverse[i] + mm(inverse[i], power[i]) for i in n]
        if step < 3:
            power = [mm(power[i], power[i]) for i in n]
    for inside, outside in ((in64, in32), (None, in64)):
        part = []
        for i in n:
            side = jnp.where(outside, 0.0, lower[i])
            part.append(side if inside is None else jnp.where(inside, side, 0.0))
        part = [mm(part[i], inverse[i]) for i in n]
        inverse = [inverse[i] - mm(inverse[i], part[i]) for i in n]
    pair = [mm(inverse[i], jnp.concatenate([ws[i] * fall, vs[i] * bs[i]], axis=1)) for i in n]
    read = [mm(scores[i], pair[i]) for i in n]
    grow = [mm(ks[i] * rest, pair[i], ((0,), (0,))) for i in n]
    reach = [qs[i] * fall - read[i][:, :DK] for i in n]
    erase = [kept * eye - grow[i][:, :DK] for i in n]
    shift = [grow[i][:, DK:] for i in n]
    state = None
    for i in n:
        out = slice(CHUNK * i, CHUNK * (i + 1))
        if state is None:
            reach_out[out, :] = reach[i].astype(BF16)
            local_out[out, :] = read[i][:, DK:]
            state = (erase[i], shift[i])
        else:
            joined = jnp.concatenate(state, axis=1)
            seen = mm(reach[i], joined)
            reach_out[out, :] = seen[:, :DK].astype(BF16)
            local_out[out, :] = seen[:, DK:] + read[i][:, DK:]
            after = mm(erase[i], joined)
            state = (after[:, :DK], after[:, DK:] + shift[i])
    maps[0] = state[0].astype(BF16)
    maps[1] = state[1].astype(BF16)


def local(rate, xf, wf, taps):
    vmem = pl.BlockSpec(memory_space=pltpu.VMEM)
    rows = PLANE * ROWS
    return pl.pallas_call(
        local_kernel,
        out_shape=(
            jax.ShapeDtypeStruct((2, DK, DK), BF16),
            jax.ShapeDtypeStruct((rows, DK), BF16),
            jax.ShapeDtypeStruct((rows, DK), F32),
            jax.ShapeDtypeStruct((rows, DK), F32),
        ),
        in_specs=[pl.BlockSpec(memory_space=pltpu.SMEM)] + [vmem] * 3,
        out_specs=(vmem,) * 4,
        scratch_shapes=[pltpu.VMEM((rows + ROWS, 3 * DK), F32)],
        name="local",
    )(rate, xf, wf, taps)


UP, DOWN = 8, 7


def finish_kernel(
    maps, reach, inner, gate, gain, woc, out, up, down, wall, gsend, gbuf, local, s_up, r_up, s_dn, r_dn, s_w, r_w, s_c, r_c, s_g, r_g
):
    z, y, x, c = place()
    tp = x * C + c
    others = [((z * Y + (y + dy) % Y), (tp + dt) % TP) for dy in range(Y) for dt in range(TP) if dy or dt]
    meet([at(z - 1, y, x, c), at(z + 1, y, x, c)] + others)
    sent = []

    def go(copy):
        copy.start()
        sent.append(copy)
        return copy

    ups, downs = {}, {}

    def send_up(d, p, src):
        i = 2 * d + p
        ups[d + 1, p] = go(remote(src, up.at[d, p], s_up.at[i], r_up.at[i], at(z + 1, y, x, c)))

    def send_down(d, p, src):
        i = 2 * d + p
        downs[d + 1, p] = go(remote(src, down.at[d, p], s_dn.at[i], r_dn.at[i], at(z - 1, y, x, c)))

    for p in range(2):
        send_up(0, p, maps.at[p])
        send_down(0, p, maps.at[p])

    def column(k):
        return wall.at[:, :, :, :, pl.ds(pl.multiple_of(((x - k + X) % X * C + c) * DK, DK), DK)]

    own = pltpu.make_async_copy(woc, column(0), local.at[0])
    own.start()
    wx = [go(remote(woc, column(0), s_w.at[k], r_w.at[k], at(z, y, x + k + 1, c))) for k in range(3)]
    wc = [go(remote(woc, column(0), s_c.at[0], r_c.at[0], at(z, y, x, c + 1)))]

    a_map = (
        lax.broadcasted_iota(jnp.int32, (DK, DK), 0) == lax.broadcasted_iota(jnp.int32, (DK, DK), 1)
    ).astype(F32)
    a_shift = jnp.zeros((DK, DK), F32)
    state = jnp.zeros((DK, DK), F32)
    for d in range(1, UP + 1):
        for p in range(2):
            ups[d, p].wait_recv()
            if d < UP:
                send_up(d, p, up.at[d - 1, p])
            if d <= DOWN:
                downs[d, p].wait_recv()
                if d < DOWN:
                    send_down(d, p, down.at[d - 1, p])
        there = d <= z
        new_shift = mm(a_map, up[d - 1, 1]) + a_shift
        new_map = mm(a_map, up[d - 1, 0])
        a_shift = jnp.where(there, new_shift, a_shift)
        a_map = jnp.where(there, new_map, a_map)
        if d <= DOWN:
            state = jnp.where(z + d >= Z, mm(down[d - 1, 0], state) + down[d - 1, 1].astype(F32), state)
    state = mm(a_map, state) + a_shift
    o = mm(reach[...], state) + inner[...]
    o = o * lax.rsqrt(jnp.mean(o * o, axis=1, keepdims=True) + out_epsilon) * gain[...] * gate[...]
    gsend[...] = o.astype(BF16).reshape(Y, TP, ROWS, DK)

    lane = pl.ds(pl.multiple_of(tp * DK, DK), DK)
    target = gbuf.at[y, :, lane]
    mine = pltpu.make_async_copy(gsend.at[y, tp], target, local.at[1])
    mine.start()
    gs = []
    for i, (sp, t) in enumerate(others):
        gs.append(go(remote(gsend.at[sp % Y, t], target, s_g.at[i], r_g.at[i], (sp, t))))

    own.wait()
    for k in range(3):
        wx[k].wait_recv()
        part = column(k + 1)
        wc.append(go(remote(part, part, s_c.at[k + 1], r_c.at[k + 1], at(z, y, x, c + 1))))
    for copy in wc:
        copy.wait_recv()
    mine.wait()
    for copy in gs:
        copy.wait_recv()
    full = lax.dot_general(
        gbuf[...].reshape(Y * ROWS, D),
        wall[...].reshape(D, D),
        (((1,), (1,)), ((), ())),
        preferred_element_type=F32,
    )
    out[...] = full.astype(BF16).reshape(Y, ROWS, D)
    for copy in sent:
        copy.wait_send()


def finish(maps, reach, inner, gate, gain, woc):
    vmem = pl.BlockSpec(memory_space=pltpu.VMEM)
    dma = pltpu.SemaphoreType.DMA
    return pl.pallas_call(
        finish_kernel,
        out_shape=jax.ShapeDtypeStruct((Y, ROWS, D), BF16),
        in_specs=[vmem] * 6,
        out_specs=vmem,
        scratch_shapes=[
            pltpu.VMEM((UP, 2, DK, DK), BF16),
            pltpu.VMEM((DOWN, 2, DK, DK), BF16),
            pltpu.VMEM((4, 4, Y, 16, D), BF16),
            pltpu.VMEM((Y, TP, ROWS, DK), BF16),
            pltpu.VMEM((Y, ROWS, D), BF16),
            dma((2,)),
            dma((2 * UP,)),
            dma((2 * UP,)),
            dma((2 * DOWN,)),
            dma((2 * DOWN,)),
            dma((3,)),
            dma((3,)),
            dma((4,)),
            dma((4,)),
            dma((PLANE - 1,)),
            dma((PLANE - 1,)),
        ],
        compiler_params=pltpu.CompilerParams(collective_id=2, has_side_effects=True),
        name="finish",
    )(maps, reach, inner, gate, gain, woc)


def rms_scale(values_in, gain):
    values = values_in.astype(F32)
    scaled = values * lax.rsqrt(jnp.mean(values * values, axis=-1, keepdims=True) + epsilon)
    return (scaled * gain).astype(BF16)


def shards(
    tokens, in_gain, w_query, w_key, w_value, w_gate, w_beta, conv_query, conv_key, conv_value, decay_rate, out_gain, w_out
):
    nrm = jnp.pad(jnp.swapaxes(rms_scale(tokens, in_gain), 0, 1), ((0, 0), (PAD, 0), (0, 0)))
    wblk = jnp.concatenate([w_query, w_key, w_value, w_gate, jnp.pad(w_beta, ((0, 0), (0, DK - 1)))], axis=1)
    taps = jnp.concatenate([conv_query, conv_key, conv_value], axis=1).astype(F32)
    xf, wf, wo = gather(nrm, wblk, w_out.T)
    maps, reach, inner, gate = local(decay_rate.reshape(1, 1), xf, wf.reshape(D, WIDE), taps)
    out = finish(maps, reach, inner, gate, out_gain.reshape(1, DK), wo)
    return jnp.swapaxes(out[:, PAD:], 0, 1)


def solution(mesh):
    both = ("sp", "tp")
    weight = P("sp", "tp")
    return jax.shard_map(
        shards,
        mesh=mesh,
        in_specs=(
            P(both, None, None),
            P(),
            weight,
            weight,
            weight,
            weight,
            weight,
            P(None, "tp"),
            P(None, "tp"),
            P(None, "tp"),
            P("tp"),
            P(),
            P("tp", "sp"),
        ),
        out_specs=P(both, None, None),
        check_vma=False,
    )
```
